32 devices in a mesh: sp: 8 (over z, x), tp: 4 (over y, core).
Axes of the slice: x: 2, y: 2, z: 4, core: 2. Of those that a mesh axis runs over, the one named last changes fastest.
Arguments:
- tokens: bfloat16 [4096, 2048], P('sp', 'tp'), may hold values from -72 to 72
- w_query: bfloat16 [2048, 1024], P('sp', 'tp'), may hold values from -0.125 to 0.125
- w_key: bfloat16 [2048, 256], P('sp', 'tp'), may hold values from -0.125 to 0.125
- w_value: bfloat16 [2048, 256], P('sp', 'tp'), may hold values from -0.125 to 0.125
- w_pool_in: bfloat16 [2048, 1024], P('sp', 'tp'), may hold values from -0.125 to 0.125
- sink: float32 [16], P('tp'), may hold values from 3 to 7
- w_pool: bfloat16 [4, 256, 256], P('tp'), may hold values from -0.375 to 0.375
- pool_scale: float32 [1024], P('tp'), may hold values from 0.1 to 1.9
- w_out_attn: bfloat16 [1024, 2048], P('tp', 'sp'), may hold values from -0.5 to 0.5
- w_out_pool: bfloat16 [1024, 2048], P('tp', 'sp'), may hold values from -0.125 to 0.125
- out_gain: float32 [2048], P('tp'), may hold values from 0.1 to 1.9
Outputs:
- mixed: bfloat16 [4096, 2048], P('sp', 'tp')
The draws below stay inside these ranges and needn't reach their ends.
All inputs are finite; a program needn't handle non-finite values.
Results may differ from the reference program's by a relative error of at most 0.012.
The reference program's roundings to bfloat16 on the way count: a program that leaves them out, or rounds other values in their place, can miss the bound.
Values may be sent and summed in bfloat16 or wider, within the bound.
A program may use at most 64 MiB of HBM per device.

```python
import jax
import jax.numpy as jnp
from jax import lax

D = 2048
HEADS = 16
KV_HEADS = 4
HEAD_DIM = 64
POOL_GROUPS = 4
GROUP_DIM = 256
WINDOW = 128
SEQ = 4096
ATTN_WIDTH = 1024
KV_WIDTH = 256
POOL_WIDTH = 1024
N_TP = 4


def draw_tokens(key, part):
    base = jnp.clip(jax.random.normal(key, (SEQ, D), jnp.float32), -6.0, 6.0)
    return base.astype(jnp.bfloat16)


def levels(stream_key, dims, pieces, smallest, top_value):
    level = 1.0
    for position, shards_of in pieces:
        heights = jax.random.uniform(jax.random.fold_in(jax.random.fold_in(stream_key, 6), position), (shards_of,), jnp.float32, smallest / len(pieces), top_value / len(pieces))
        level = level * jnp.repeat(jnp.exp(heights), dims[position] // shards_of).reshape((-1,) + (1,) * (len(dims) - 1 - position))
    return level


def centred(rng, shape, deviation, bound, shards=(), kind=jnp.bfloat16):
    entries = jax.random.normal(rng, shape, jnp.float32) * deviation
    if len(shards) > 0:
        entries = levels(rng, shape, shards, -0.22, 0.18) * entries
    return jnp.clip(entries, min=-bound, max=bound).astype(kind)


def setup_inputs(seed: int = 0) -> dict:
    splits = jax.random.split(jax.random.key(seed), 12)
    return {
        "tokens": draw_tokens(jax.random.fold_in(splits[11], 71), 0),
        "w_query": centred(splits[1], (D, ATTN_WIDTH), D ** -0.5, 0.125, ((0, 8), (1, 4))),
        "w_key": centred(splits[2], (D, KV_WIDTH), D ** -0.5, 0.125, ((0, 8), (1, 4))),
        "w_value": centred(splits[3], (D, KV_WIDTH), D ** -0.5, 0.125, ((0, 8), (1, 4))),
        "w_pool_in": centred(splits[4], (D, POOL_WIDTH), D ** -0.5, 0.125, ((0, 8), (1, 4))),
        "sink": jnp.clip(3.0 + 4.0 * jax.random.uniform(splits[5], (HEADS,), jnp.float32) ** levels(splits[5], (HEADS,), ((0, 4),), -0.2, 0.2), 3.0, 7.0),
        "w_pool": centred(splits[6], (POOL_GROUPS, GROUP_DIM, GROUP_DIM), GROUP_DIM ** -0.5, 0.375, ((0, 4),)),
        "pool_scale": jnp.clip(1.0 + 0.18 * jax.random.normal(splits[7], (POOL_WIDTH,), jnp.float32), 0.1, 1.9),
        "w_out_attn": centred(splits[8], (ATTN_WIDTH, D), (ATTN_WIDTH // 8) ** -0.5, 0.5, ((0, 4), (1, 8))),
        "w_out_pool": centred(splits[9], (POOL_WIDTH, D), (ATTN_WIDTH + POOL_WIDTH) ** -0.5, 0.125, ((0, 4), (1, 8))),
        "out_gain": jnp.clip(1.0 + 0.18 * jax.random.normal(splits[10], (D,), jnp.float32), 0.1, 1.9),
    }


epsilon = 1e-05
masked_score = -1e+30

def attend_head(query_one, key_one, value_one, sink_one):
    seq_len = query_one.shape[0]
    group = query_one.shape[1]
    block_count = seq_len // WINDOW
    query_blocks = query_one.reshape(block_count, WINDOW, group, HEAD_DIM).astype(jnp.float32)

    def banded(source):
        padded = jnp.pad(source, ((WINDOW, WINDOW), (0, 0))).reshape(block_count + 2, WINDOW, HEAD_DIM)
        return jnp.concatenate([padded[:-2], padded[1:-1], padded[2:]], axis=1).astype(jnp.float32)
    key_band = banded(key_one)
    value_band = banded(value_one)
    scores = jnp.einsum('nqgd,nsd->ngqs', query_blocks, key_band) * HEAD_DIM ** (-0.5)
    starts = jnp.arange(block_count, dtype=jnp.int32) * WINDOW
    query_pos = starts[:, None] + jnp.arange(WINDOW, dtype=jnp.int32)[None, :]
    key_pos = starts[:, None] + jnp.arange(3 * WINDOW, dtype=jnp.int32)[None, :] - WINDOW
    distance = key_pos[:, None, :] - query_pos[:, :, None]
    inside = (key_pos >= 0) & (key_pos < seq_len)
    keep = (jnp.abs(distance) <= WINDOW) & inside[:, None, :]
    scores = jnp.where(keep[:, None], scores, masked_score)
    sink_logit = sink_one.astype(jnp.float32)[None, :, None, None]
    top = jnp.maximum(lax.optimization_barrier(jnp.max(scores, axis=-1, keepdims=True)), sink_logit)
    raised = jnp.exp(scores - top)
    total = lax.optimization_barrier(jnp.sum(raised, axis=-1, keepdims=True)) + jnp.exp(sink_logit - top)
    probs = (raised / total).astype(jnp.bfloat16)
    attended = jnp.einsum('ngqs,nsd->nqgd', probs.astype(jnp.float32), value_band)
    return attended.astype(jnp.bfloat16).reshape(seq_len, group * HEAD_DIM)

def reference(tokens, w_query, w_key, w_value, w_pool_in, sink, w_pool, pool_scale, w_out_attn, w_out_pool, out_gain):
    seq_len = tokens.shape[0]
    group = HEADS // KV_HEADS
    query = jnp.dot(tokens, w_query, preferred_element_type=jnp.float32).astype(jnp.bfloat16)
    keys = jnp.dot(tokens, w_key, preferred_element_type=jnp.float32).astype(jnp.bfloat16)
    values = jnp.dot(tokens, w_value, preferred_element_type=jnp.float32).astype(jnp.bfloat16)
    chan = jnp.dot(tokens, w_pool_in, preferred_element_type=jnp.float32).astype(jnp.bfloat16)
    query_heads = query.reshape(seq_len, KV_HEADS, group, HEAD_DIM).transpose(1, 0, 2, 3)
    key_heads = keys.reshape(seq_len, KV_HEADS, HEAD_DIM).transpose(1, 0, 2)
    value_heads = values.reshape(seq_len, KV_HEADS, HEAD_DIM).transpose(1, 0, 2)
    sink_heads = sink.reshape(KV_HEADS, group)
    attended = lax.map(lambda parts: attend_head(*parts), (query_heads, key_heads, value_heads, sink_heads))
    attended = attended.transpose(1, 0, 2).reshape(seq_len, HEADS * HEAD_DIM)
    chan_float = chan.astype(jnp.float32)
    running = jnp.concatenate([jnp.zeros((1, POOL_WIDTH), jnp.float32), jnp.cumsum(chan_float, axis=0)], axis=0)
    positions = jnp.arange(seq_len, dtype=jnp.int32)
    outputs = []
    for level in range(POOL_GROUPS):
        half = 2 ** level
        lower = jnp.clip(positions - half, 0, seq_len)
        upper = jnp.clip(positions + half, 0, seq_len)
        columns = slice(level * GROUP_DIM, (level + 1) * GROUP_DIM)
        band = running[:, columns]
        count = (upper - lower).astype(jnp.float32)
        spread = ((band[upper] - band[lower]) / count[:, None] - chan_float[:, columns]).astype(jnp.bfloat16)
        outputs.append(jnp.dot(spread, w_pool[level], preferred_element_type=jnp.float32))
    pooled = (jnp.concatenate(outputs, axis=1) * pool_scale).astype(jnp.bfloat16)
    attn_share = ATTN_WIDTH // N_TP
    pool_share = POOL_WIDTH // N_TP
    mix = jnp.zeros((seq_len, D), jnp.float32)
    for device in range(N_TP):
        attn_cols = slice(device * attn_share, (device + 1) * attn_share)
        pool_cols = slice(device * pool_share, (device + 1) * pool_share)
        partial_sum = jnp.dot(attended[:, attn_cols], w_out_attn[attn_cols], preferred_element_type=jnp.float32)
        partial_sum = partial_sum + jnp.dot(pooled[:, pool_cols], w_out_pool[pool_cols], preferred_element_type=jnp.float32)
        mix = mix + partial_sum.astype(jnp.bfloat16).astype(jnp.float32)
    row_mean = lax.optimization_barrier(jnp.sum(mix, axis=1)) / D
    variance = lax.optimization_barrier(jnp.sum(mix * mix, axis=1)) / D - row_mean * row_mean
    normed = (mix - row_mean[:, None]) * lax.rsqrt(variance + epsilon)[:, None] * out_gain
    return normed.astype(jnp.bfloat16)
```

```python
import functools

import jax
import jax.numpy as jnp
from jax import lax
from jax.experimental import pallas as pl
from jax.experimental.pallas import tpu as pltpu
from jax.sharding import PartitionSpec as P

HEAD_DIM = 64
POOL_GROUPS = 4
WINDOW = 128


epsilon = 1e-05
masked_score = -1e30


def padded(cells, sides, width):
    for axis, dim in sides:
        count = lax.axis_size(axis)
        ends = count - 1
        head = lax.slice_in_dim(cells, 0, width, axis=dim)
        tail = lax.slice_in_dim(cells, cells.shape[dim] - width, cells.shape[dim], axis=dim)
        cells = jnp.concatenate(
            [
                lax.ppermute(tail, axis, [(i, (i + 1) % count) for i in range(ends)]),
                cells,
                lax.ppermute(head, axis, [((i + 1) % count, i) for i in range(ends)]),
            ],
            axis=dim,
        )
    return cells


def make_projector(gathered, pieces):
    piece_query, piece_key, piece_value, piece_chan = pieces
    joined = jnp.concatenate([piece_key, piece_value], axis=1)
    return (
        jnp.dot(gathered, piece_query, preferred_element_type=jnp.float32),
        jnp.dot(gathered, joined, preferred_element_type=jnp.float32),
        jnp.dot(gathered, piece_chan, preferred_element_type=jnp.float32),
    )


def attend_local(query, keys_ext, sinks, offset, seq_len, key_cols):
    tok_rows, query_cols = query.shape
    kv_local = key_cols // HEAD_DIM
    group = query_cols // key_cols
    block_count = tok_rows // WINDOW
    stacked = keys_ext.reshape(block_count + 2, WINDOW, 2 * key_cols)
    banded = jnp.concatenate([stacked[:-2], stacked[1:-1], stacked[2:]], axis=1)
    key_band = banded[:, :, :key_cols].reshape(block_count, 3 * WINDOW, kv_local, HEAD_DIM)
    value_band = banded[:, :, key_cols:].reshape(block_count, 3 * WINDOW, kv_local, HEAD_DIM)
    query_blocks = query.reshape(block_count, WINDOW, kv_local, group, HEAD_DIM)
    scores = jnp.einsum(
        "nqkgd,nskd->nkgqs", query_blocks, key_band, preferred_element_type=jnp.float32
    ) * HEAD_DIM ** (-0.5)
    starts = offset + jnp.arange(block_count, dtype=jnp.int32) * WINDOW
    query_pos = starts[:, None] + jnp.arange(WINDOW, dtype=jnp.int32)[None, :]
    key_pos = starts[:, None] + jnp.arange(3 * WINDOW, dtype=jnp.int32)[None, :] - WINDOW
    distance = key_pos[:, None, :] - query_pos[:, :, None]
    inside = (key_pos >= 0) & (key_pos < seq_len)
    keep = (jnp.abs(distance) <= WINDOW) & inside[:, None, :]
    scores = jnp.where(keep[:, None, None], scores, masked_score)
    sink_logit = sinks.reshape(kv_local, group)[None, :, :, None, None]
    top = jnp.maximum(jnp.max(scores, axis=-1, keepdims=True), sink_logit)
    raised = jnp.exp(scores - top)
    total = jnp.sum(raised, axis=-1, keepdims=True) + jnp.exp(sink_logit - top)
    probs = (raised / total).astype(jnp.bfloat16)
    attended = jnp.einsum(
        "nkgqs,nskd->nqkgd", probs, value_band, preferred_element_type=jnp.float32
    )
    return attended.astype(jnp.bfloat16).reshape(tok_rows, query_cols)


def local(
    tokens,
    w_query,
    w_key,
    w_value,
    w_pool_in,
    sink,
    w_pool,
    pool_scale,
    w_out_attn,
    w_out_pool,
    out_gain,
):
    tok_rows = tokens.shape[0]
    seq_len = tok_rows * lax.axis_size("sp")
    offset = lax.axis_index("sp") * tok_rows
    out_both = jnp.concatenate([w_out_attn, w_out_pool], axis=0)
    gathered = lax.all_gather(tokens, "tp", axis=1, tiled=True)
    key_cols = w_key.shape[1]
    chan_cols = w_pool_in.shape[1]
    query_sum, joined_sum, chan_sum = make_projector(
        gathered,
        (
            lax.all_gather(w_query, "sp", axis=0, tiled=True),
            lax.all_gather(w_key, "sp", axis=0, tiled=True),
            lax.all_gather(w_value, "sp", axis=0, tiled=True),
            lax.all_gather(w_pool_in, "sp", axis=0, tiled=True),
        ),
    )
    query = query_sum.astype(jnp.bfloat16)
    key_value = joined_sum.astype(jnp.bfloat16)
    chan = chan_sum.astype(jnp.bfloat16)
    keys_ext = padded(key_value, (("sp", 0),), WINDOW)
    attended = attend_local(query, keys_ext, sink, offset, seq_len, key_cols)
    rim_rows = 2 ** (POOL_GROUPS - 1)
    chan_ext = padded(chan, (("sp", 0),), rim_rows)
    running = jnp.concatenate(
        [jnp.zeros((1, chan_cols), jnp.float32), jnp.cumsum(chan_ext.astype(jnp.float32), axis=0)],
        axis=0,
    )
    chan_float = chan.astype(jnp.float32)
    positions = offset + jnp.arange(tok_rows, dtype=jnp.int32)
    group_count = w_pool.shape[0]
    level = lax.axis_index("tp") * group_count + 0
    half = jnp.left_shift(jnp.int32(1), level)
    upper = lax.dynamic_slice_in_dim(running, rim_rows + half, tok_rows, 0)
    lower = lax.dynamic_slice_in_dim(running, rim_rows - half, tok_rows, 0)
    count = (
        jnp.clip(positions + half, 0, seq_len) - jnp.clip(positions - half, 0, seq_len)
    ).astype(jnp.float32)
    spread = ((upper - lower) / count[:, None] - chan_float).astype(jnp.bfloat16)
    outputs = jnp.dot(spread, w_pool[0], preferred_element_type=jnp.float32)
    pooled = (outputs * pool_scale).astype(jnp.bfloat16)
    hidden = jnp.concatenate([attended, pooled], axis=1)
    terms = jnp.dot(
        hidden,
        lax.all_gather(out_both, "sp", axis=1, tiled=True),
        preferred_element_type=jnp.float32,
    )
    share_width = out_gain.shape[0]
    model_width = share_width * lax.axis_size("tp")
    share = lax.psum_scatter(
        terms.astype(jnp.bfloat16), "tp", scatter_dimension=1, tiled=True
    ).astype(jnp.float32)
    row_total, row_square = lax.psum((jnp.sum(share, axis=1), jnp.sum(share * share, axis=1)), "tp")
    row_mean = row_total / model_width
    variance = row_square / model_width - row_mean * row_mean
    normed = (share - row_mean[:, None]) * lax.rsqrt(variance + epsilon)[:, None] * out_gain
    return normed.astype(jnp.bfloat16)


MESH = pl.DeviceIdType.MESH
RIM = 16


def mixer_kernel(
    n,
    tp,
    tok_ref,
    wq_ref,
    wk_ref,
    wv_ref,
    wc_ref,
    sink_ref,
    wp_ref,
    ps_ref,
    woa_ref,
    wop_ref,
    gain_ref,
    out_ref,
    win,
    wout,
    tok,
    acc,
    query,
    kv,
    chan,
    hidden,
    part,
    landed,
    stats,
    win_send,
    win_recv,
    wout_send,
    wout_recv,
    tok_send,
    tok_recv,
    rim_send,
    rim_recv,
    part_send,
    part_recv,
    stat_send,
    stat_recv,
):
    f32, bf16 = jnp.float32, jnp.bfloat16
    me, t = lax.axis_index("sp"), lax.axis_index("tp")
    rows = tok_ref.shape[0]
    seq_len = rows * n
    half_n = n // 2
    column = me % 2
    pos = (me // 2) * (1 - column) + column * (n - 1 - me // 2)

    def at(p):
        p = lax.rem(p + n, n)
        back = p // half_n
        return (1 - back) * (2 * p) + back * (2 * (n - 1 - p) + 1)

    ring = (at(pos + 1), at(pos - 1))
    after, before = lax.rem(me + 1, n), lax.rem(me + n - 1, n)
    mate = t + 1 - 2 * lax.rem(t, 2)
    across = lax.rem(t + 2, tp)
    per = n // tp

    def rdma(src, dst, send, recv, sp, tpi):
        return pltpu.make_async_remote_copy(
            src_ref=src,
            dst_ref=dst,
            send_sem=send,
            recv_sem=recv,
            device_id={"sp": sp, "tp": tpi},
            device_id_type=MESH,
        )

    qc, kc = wq_ref.shape[1], wk_ref.shape[1]
    cc = wc_ref.shape[1]
    depth = wq_ref.shape[0]
    hd = depth // 2
    for h in range(2):
        r = slice(h * hd, (h + 1) * hd)
        win[me, h, :, 0:qc] = wq_ref[r, :]
        win[me, h, :, qc : qc + 2 * kc] = jnp.concatenate([wk_ref[r, :], wv_ref[r, :]], axis=1)
        win[me, h, :, qc + 2 * kc :] = wc_ref[r, :]
    for b in range(per):
        tok[t * per + b] = tok_ref[:, b * depth : (b + 1) * depth]
    wout[me, 0] = woa_ref[...]
    wout[me, 1] = wop_ref[...]

    barrier = pltpu.get_barrier_semaphore()
    peers = [(s, t) for s in ring] + [(s, t) for s in (before, after)]
    peers += [(me, lax.rem(t + i, tp)) for i in range(1, tp)]
    for s, p in peers:
        pl.semaphore_signal(barrier, inc=1, device_id={"sp": s, "tp": p}, device_id_type=MESH)
    pl.semaphore_wait(barrier, len(peers))

    def ring_copy(buf, send, recv, way, k, hop):
        sign = -1 if way == 0 else 1
        h = k % 2 if way == 0 else 1 - k % 2
        slot = buf.at[at(pos + sign * (k // 2 + hop)), h]
        return rdma(slot, slot, send.at[way, k], recv.at[way, k], ring[way], t)

    def w_in(way, k, hop):
        return ring_copy(win, win_send, win_recv, way, k, hop)

    def w_out(way, k, hop):
        return ring_copy(wout, wout_send, wout_recv, way, k, hop)

    def tok_copy(owner, b, i, dst):
        slot = tok.at[owner * per + b]
        return rdma(slot, slot, tok_send.at[i], tok_recv.at[i], me, dst)

    for b in range(per):
        tok_copy(t, b, b, across).start()
        for way in range(2):
            if b < 2:
                w_in(way, b, 0).start()
    for b in range(per):
        tok_copy(t, b, per + b, mate).start()

    last = n - 2
    origin = [at(pos)]
    for d in range(1, half_n):
        origin += [at(pos - d), at(pos + d)]
    origin.append(at(pos + half_n))

    def project(i, first=False):
        o = origin[i]
        w = win[o].reshape(depth, qc + 2 * kc + cc)
        term = jnp.dot(tok[o], w, preferred_element_type=f32)
        if first:
            acc[...] = term
        else:
            acc[...] += term

    def relay(copy, k, after_last):
        for way in range(2):
            copy(way, k, 1).wait_recv()
            if k + 2 <= last:
                copy(way, k + 2, 0).start()
            elif after_last is not None:
                after_last(way, k + 1 - last)

    def start_out(way, k):
        w_out(way, k, 0).start()

    ready = 0
    done_blocks = 0
    tok_step = {1: 0, 3: 1}
    tokens_here = False
    for k in range(last + 1):
        relay(w_in, k, start_out)
        if k in tok_step:
            b = tok_step[k]
            tok_copy(across, b, b, across).wait_recv()
            tok_copy(across, b, 2 * per + b, mate).start()
        if k == 3:
            for b in range(per):
                tok_copy(mate, b, per + b, mate).wait_recv()
                tok_copy(lax.rem(mate + 2, tp), b, 2 * per + b, mate).wait_recv()
            tokens_here = True
        ready = 1 + 2 * ((k + 1) // 2) if k < last else n
        if tokens_here:
            while done_blocks < ready and (k == last or done_blocks < 1 + 2 * ((k - 2) // 1)):
                project(done_blocks, done_blocks == 0)
                done_blocks += 1

    query[...] = acc[:, 0:qc].astype(bf16)
    kv[WINDOW : WINDOW + rows, :] = acc[:, qc : qc + 2 * kc].astype(bf16)
    chan[RIM : RIM + rows, :] = acc[:, qc + 2 * kc :].astype(bf16)

    def rim(buf, width, down, i):
        if down:
            return rdma(buf.at[pl.ds(rows, width)], buf.at[pl.ds(0, width)], rim_send.at[i], rim_recv.at[i], after, t)
        return rdma(
            buf.at[pl.ds(width, width)], buf.at[pl.ds(rows + width, width)], rim_send.at[i], rim_recv.at[i], before, t
        )

    rims = [rim(kv, WINDOW, True, 0), rim(kv, WINDOW, False, 1), rim(chan, RIM, True, 2), rim(chan, RIM, False, 3)]
    for c in rims:
        c.start()

    group = qc // kc

    def attend(b):
        band = kv[b * WINDOW : (b + 3) * WINDOW, :]
        q = query[b * WINDOW : (b + 1) * WINDOW, :]
        stacked = jnp.concatenate([q[:, g * HEAD_DIM : (g + 1) * HEAD_DIM] for g in range(group)], axis=0)
        scores = lax.dot_general(
            stacked, band[:, :HEAD_DIM], (((1,), (1,)), ((), ())), preferred_element_type=f32
        ) * HEAD_DIM ** (-0.5)
        scores = scores.reshape(group, WINDOW, 3 * WINDOW)
        r = lax.broadcasted_iota(jnp.int32, (WINDOW, 3 * WINDOW), 0)
        c = lax.broadcasted_iota(jnp.int32, (WINDOW, 3 * WINDOW), 1)
        keep = (c >= r) & (c <= r + 2 * WINDOW)
        key_pos = c + (me * rows + b * WINDOW - WINDOW)
        keep = keep & (key_pos >= 0) & (key_pos < seq_len)
        outs = []
        for g in range(group):
            s = jnp.where(keep, scores[g], masked_score)
            logit = sink_ref[0, g]
            top = jnp.maximum(jnp.max(s, axis=1, keepdims=True), logit)
            raised = jnp.exp(s - top)
            total = jnp.sum(raised, axis=1, keepdims=True) + jnp.exp(logit - top)
            outs.append((raised * (1.0 / total)).astype(bf16))
        got = jnp.dot(jnp.concatenate(outs, axis=0), band, preferred_element_type=f32)
        got = got[:, HEAD_DIM : 2 * HEAD_DIM].astype(bf16)
        hidden[b * WINDOW : (b + 1) * WINDOW, 0:qc] = jnp.concatenate(
            [got[g * WINDOW : (g + 1) * WINDOW] for g in range(group)], axis=1
        )

    def pool():
        length = rows + 2 * RIM
        e = chan[...].astype(f32)
        p = lax.broadcasted_iota(jnp.int32, (length, 1), 0) + (me * rows - RIM)
        e = jnp.where((p >= 0) & (p < seq_len), e, 0.0)
        sums = e + pltpu.roll(e, 1, 0)
        pick = sums
        for level in range(1, POOL_GROUPS):
            step = 2 ** (level - 1)
            sums = pltpu.roll(sums, step, 0) + pltpu.roll(sums, length - step, 0)
            pick = jnp.where(t == level, sums, pick)
        half = 1
        for level in range(1, POOL_GROUPS):
            half = jnp.where(t == level, 2**level, half)
        count = (jnp.clip(p + half, 0, seq_len) - jnp.clip(p - half, 0, seq_len)).astype(f32)
        spread = (pick[RIM : RIM + rows] / count[RIM : RIM + rows] - e[RIM : RIM + rows]).astype(bf16)
        got = jnp.dot(spread, wp_ref[0], preferred_element_type=f32)
        hidden[:, qc:] = (got * ps_ref[...]).astype(bf16)

    def part_copy(o, src):
        s = lax.rem(o, per)
        owner = o // per
        return rdma(
            part.at[o], landed.at[src, s], part_send.at[o], part_recv.at[src, s], me, owner
        )

    def emit(i):
        o = origin[i]
        got = jnp.dot(hidden[:, 0:qc], wout[o, 0], preferred_element_type=f32)
        got = got + jnp.dot(hidden[:, qc:], wout[o, 1], preferred_element_type=f32)
        part[o] = got.astype(bf16)

        @pl.when(o // per != t)
        def _():
            part_copy(o, t).start()

    blocks = rows // WINDOW
    relay(w_out, 0, None)
    for b in range(1, blocks - 1):
        attend(b)
    relay(w_out, 1, None)
    for c in rims:
        c.wait()
    pool()
    relay(w_out, 2, None)
    attend(0)
    relay(w_out, 3, None)
    attend(blocks - 1)
    for i in range(0, 5):
        emit(i)
    for k in range(4, last + 1):
        relay(w_out, k, None)
        if k % 2 == 1:
            emit(k)
            emit(k + 1)
    emit(n - 1)

    share = []
    for s in range(per):
        total = part[t * per + s].astype(f32)
        for j in range(1, tp):
            src = lax.rem(t + j, tp)
            rdma(
                landed.at[src, s], landed.at[src, s], part_send.at[t * per + s], part_recv.at[src, s], me, src
            ).wait_recv()
            total = total + landed[src, s].astype(f32)
        share.append(total)
    mix = jnp.concatenate(share, axis=1)
    acc[:, 0 : mix.shape[1]] = mix
    one = jnp.sum(mix, axis=1, keepdims=True)
    two = jnp.sum(mix * mix, axis=1, keepdims=True)
    lane = lax.broadcasted_iota(jnp.int32, (rows, 128), 1)
    both = jnp.where(lane == 0, one, jnp.where(lane == 1, two, 0.0))
    stats[t] = jnp.transpose(both)[0:8]

    def stat_copy(j):
        return rdma(stats.at[t], stats.at[t], stat_send.at[j], stat_recv.at[t], me, lax.rem(t + j, tp))

    for j in range(1, tp):
        stat_copy(j).start()
    for o in range(n):

        @pl.when(o // per != t)
        def _():
            part_copy(o, t).wait_send()

    for k in range(last + 1):
        for way in range(2):
            w_in(way, k, 0).wait_send()
            w_out(way, k, 0).wait_send()
    for b in range(per):
        tok_copy(t, b, b, across).wait_send()
        tok_copy(t, b, per + b, mate).wait_send()
        tok_copy(across, b, 2 * per + b, mate).wait_send()
    for j in range(1, tp):
        src = lax.rem(t + j, tp)
        rdma(stats.at[src], stats.at[src], stat_send.at[j], stat_recv.at[src], me, src).wait_recv()
    totals = stats[0]
    for i in range(1, tp):
        totals = totals + stats[i]
    wide = jnp.concatenate([totals, jnp.zeros((120, rows), f32)], axis=0)
    back = jnp.transpose(wide)
    width = gain_ref.shape[1] * tp
    row_mean = back[:, 0:1] / width
    variance = back[:, 1:2] / width - row_mean * row_mean
    scale = lax.rsqrt(variance + epsilon)
    out_ref[...] = ((acc[:, 0 : gain_ref.shape[1]] - row_mean) * scale * gain_ref[...]).astype(bf16)
    for j in range(1, tp):
        stat_copy(j).wait_send()


def fused(n, tp, tokens, w_query, w_key, w_value, w_pool_in, sink, w_pool, pool_scale, w_out_attn, w_out_pool, out_gain):
    rows, share = tokens.shape
    depth, qc = w_query.shape
    kc, cc = w_key.shape[1], w_pool_in.shape[1]
    wide = w_out_attn.shape[1]
    per = n // tp
    bf16, f32 = jnp.bfloat16, jnp.float32
    dma = pltpu.SemaphoreType.DMA
    vmem = pl.BlockSpec(memory_space=pltpu.VMEM)
    specs = [vmem] * 11
    specs[5] = pl.BlockSpec(memory_space=pltpu.SMEM)
    return pl.pallas_call(
        functools.partial(mixer_kernel, n, tp),
        out_shape=jax.ShapeDtypeStruct((rows, share), bf16),
        in_specs=specs,
        out_specs=vmem,
        scratch_shapes=[
            pltpu.VMEM((n, 2, depth // 2, qc + 2 * kc + cc), bf16),
            pltpu.VMEM((n, 2, qc, wide), bf16),
            pltpu.VMEM((n, rows, depth), bf16),
            pltpu.VMEM((rows, qc + 2 * kc + cc), f32),
            pltpu.VMEM((rows, qc), bf16),
            pltpu.VMEM((rows + 2 * WINDOW, 2 * kc), bf16),
            pltpu.VMEM((rows + 2 * RIM, cc), bf16),
            pltpu.VMEM((rows, qc + cc), bf16),
            pltpu.VMEM((n, rows, wide), bf16),
            pltpu.VMEM((tp, per, rows, wide), bf16),
            pltpu.VMEM((tp, 8, rows), f32),
            dma((2, n - 1)),
            dma((2, n - 1)),
            dma((2, n - 1)),
            dma((2, n - 1)),
            dma((3 * per,)),
            dma((3 * per,)),
            dma((4,)),
            dma((4,)),
            dma((n,)),
            dma((tp, per)),
            dma((tp,)),
            dma((tp,)),
        ],
        compiler_params=pltpu.CompilerParams(
            collective_id=0, has_side_effects=True, vmem_limit_bytes=60 * 1024 * 1024
        ),
        name="mixer",
    )(
        tokens,
        w_query,
        w_key,
        w_value,
        w_pool_in,
        sink.reshape(1, -1),
        w_pool,
        pool_scale.reshape(1, -1),
        w_out_attn,
        w_out_pool,
        out_gain.reshape(1, -1),
    )


def fits(n, tp, tokens, w_query, w_key, w_pool, w_out_attn):
    return (
        tp == 4
        and n == 2 * tp
        and w_query.shape[0] % 32 == 0
        and w_query.shape[1] % 128 == 0
        and w_key.shape[1] == HEAD_DIM
        and w_pool.shape[0] == 1
        and w_out_attn.shape[1] % 128 == 0
        and tokens.shape[0] >= 2 * WINDOW
    )


def mixed_rows(*args):
    n, tp = lax.axis_size("sp"), lax.axis_size("tp")
    if fits(n, tp, args[0], args[1], args[2], args[6], args[8]):
        return fused(n, tp, *args)
    return local(*args)


def solution(mesh):
    return jax.shard_map(
        mixed_rows,
        mesh=mesh,
        in_specs=(
            P("sp", "tp"),
            P("sp", "tp"),
            P("sp", "tp"),
            P("sp", "tp"),
            P("sp", "tp"),
            P("tp"),
            P("tp", None, None),
            P("tp"),
            P("tp", "sp"),
            P("tp", "sp"),
            P("tp"),
        ),
        out_specs=P("sp", "tp"),
        check_vma=False,
    )
```

```python
import functools

import jax
import jax.numpy as jnp
from jax import lax
from jax.experimental import pallas as pl
from jax.experimental.pallas import tpu as pltpu
from jax.sharding import PartitionSpec as P

HEAD_DIM = 64
POOL_GROUPS = 4
WINDOW = 128


epsilon = 1e-05
masked_score = -1e30


def padded(cells, sides, width):
    for axis, dim in sides:
        count = lax.axis_size(axis)
        ends = count - 1
        head = lax.slice_in_dim(cells, 0, width, axis=dim)
        tail = lax.slice_in_dim(cells, cells.shape[dim] - width, cells.shape[dim], axis=dim)
        cells = jnp.concatenate(
            [
                lax.ppermute(tail, axis, [(i, (i + 1) % count) for i in range(ends)]),
                cells,
                lax.ppermute(head, axis, [((i + 1) % count, i) for i in range(ends)]),
            ],
            axis=dim,
        )
    return cells


def make_projector(gathered, pieces):
    piece_query, piece_key, piece_value, piece_chan = pieces
    joined = jnp.concatenate([piece_key, piece_value], axis=1)
    return (
        jnp.dot(gathered, piece_query, preferred_element_type=jnp.float32),
        jnp.dot(gathered, joined, preferred_element_type=jnp.float32),
        jnp.dot(gathered, piece_chan, preferred_element_type=jnp.float32),
    )


def attend_local(query, keys_ext, sinks, offset, seq_len, key_cols):
    tok_rows, query_cols = query.shape
    kv_local = key_cols // HEAD_DIM
    group = query_cols // key_cols
    block_count = tok_rows // WINDOW
    stacked = keys_ext.reshape(block_count + 2, WINDOW, 2 * key_cols)
    banded = jnp.concatenate([stacked[:-2], stacked[1:-1], stacked[2:]], axis=1)
    key_band = banded[:, :, :key_cols].reshape(block_count, 3 * WINDOW, kv_local, HEAD_DIM)
    value_band = banded[:, :, key_cols:].reshape(block_count, 3 * WINDOW, kv_local, HEAD_DIM)
    query_blocks = query.reshape(block_count, WINDOW, kv_local, group, HEAD_DIM)
    scores = jnp.einsum(
        "nqkgd,nskd->nkgqs", query_blocks, key_band, preferred_element_type=jnp.float32
    ) * HEAD_DIM ** (-0.5)
    starts = offset + jnp.arange(block_count, dtype=jnp.int32) * WINDOW
    query_pos = starts[:, None] + jnp.arange(WINDOW, dtype=jnp.int32)[None, :]
    key_pos = starts[:, None] + jnp.arange(3 * WINDOW, dtype=jnp.int32)[None, :] - WINDOW
    distance = key_pos[:, None, :] - query_pos[:, :, None]
    inside = (key_pos >= 0) & (key_pos < seq_len)
    keep = (jnp.abs(distance) <= WINDOW) & inside[:, None, :]
    scores = jnp.where(keep[:, None, None], scores, masked_score)
    sink_logit = sinks.reshape(kv_local, group)[None, :, :, None, None]
    top = jnp.maximum(jnp.max(scores, axis=-1, keepdims=True), sink_logit)
    raised = jnp.exp(scores - top)
    total = jnp.sum(raised, axis=-1, keepdims=True) + jnp.exp(sink_logit - top)
    probs = (raised / total).astype(jnp.bfloat16)
    attended = jnp.einsum(
        "nkgqs,nskd->nqkgd", probs, value_band, preferred_element_type=jnp.float32
    )
    return attended.astype(jnp.bfloat16).reshape(tok_rows, query_cols)


def local(
    tokens,
    w_query,
    w_key,
    w_value,
    w_pool_in,
    sink,
    w_pool,
    pool_scale,
    w_out_attn,
    w_out_pool,
    out_gain,
):
    tok_rows = tokens.shape[0]
    seq_len = tok_rows * lax.axis_size("sp")
    offset = lax.axis_index("sp") * tok_rows
    out_both = jnp.concatenate([w_out_attn, w_out_pool], axis=0)
    gathered = lax.all_gather(tokens, "tp", axis=1, tiled=True)
    key_cols = w_key.shape[1]
    chan_cols = w_pool_in.shape[1]
    query_sum, joined_sum, chan_sum = make_projector(
        gathered,
        (
            lax.all_gather(w_query, "sp", axis=0, tiled=True),
            lax.all_gather(w_key, "sp", axis=0, tiled=True),
            lax.all_gather(w_value, "sp", axis=0, tiled=True),
            lax.all_gather(w_pool_in, "sp", axis=0, tiled=True),
        ),
    )
    query = query_sum.astype(jnp.bfloat16)
    key_value = joined_sum.astype(jnp.bfloat16)
    chan = chan_sum.astype(jnp.bfloat16)
    keys_ext = padded(key_value, (("sp", 0),), WINDOW)
    attended = attend_local(query, keys_ext, sink, offset, seq_len, key_cols)
    rim_rows = 2 ** (POOL_GROUPS - 1)
    chan_ext = padded(chan, (("sp", 0),), rim_rows)
    running = jnp.concatenate(
        [jnp.zeros((1, chan_cols), jnp.float32), jnp.cumsum(chan_ext.astype(jnp.float32), axis=0)],
        axis=0,
    )
    chan_float = chan.astype(jnp.float32)
    positions = offset + jnp.arange(tok_rows, dtype=jnp.int32)
    group_count = w_pool.shape[0]
    level = lax.axis_index("tp") * group_count + 0
    half = jnp.left_shift(jnp.int32(1), level)
    upper = lax.dynamic_slice_in_dim(running, rim_rows + half, tok_rows, 0)
    lower = lax.dynamic_slice_in_dim(running, rim_rows - half, tok_rows, 0)
    count = (
        jnp.clip(positions + half, 0, seq_len) - jnp.clip(positions - half, 0, seq_len)
    ).astype(jnp.float32)
    spread = ((upper - lower) / count[:, None] - chan_float).astype(jnp.bfloat16)
    outputs = jnp.dot(spread, w_pool[0], preferred_element_type=jnp.float32)
    pooled = (outputs * pool_scale).astype(jnp.bfloat16)
    hidden = jnp.concatenate([attended, pooled], axis=1)
    terms = jnp.dot(
        hidden,
        lax.all_gather(out_both, "sp", axis=1, tiled=True),
        preferred_element_type=jnp.float32,
    )
    share_width = out_gain.shape[0]
    model_width = share_width * lax.axis_size("tp")
    share = lax.psum_scatter(
        terms.astype(jnp.bfloat16), "tp", scatter_dimension=1, tiled=True
    ).astype(jnp.float32)
    row_total, row_square = lax.psum((jnp.sum(share, axis=1), jnp.sum(share * share, axis=1)), "tp")
    row_mean = row_total / model_width
    variance = row_square / model_width - row_mean * row_mean
    normed = (share - row_mean[:, None]) * lax.rsqrt(variance + epsilon)[:, None] * out_gain
    return normed.astype(jnp.bfloat16)


MESH = pl.DeviceIdType.MESH
RIM = 16


def mixer_kernel(
    n,
    tp,
    tok_ref,
    wq_ref,
    wk_ref,
    wv_ref,
    wc_ref,
    sink_ref,
    wp_ref,
    ps_ref,
    woa_ref,
    wop_ref,
    gain_ref,
    out_ref,
    win,
    wout,
    tok,
    acc,
    query,
    kv,
    chan,
    hidden,
    part,
    mated,
    landed,
    own,
    stats,
    win_send,
    win_recv,
    wout_send,
    wout_recv,
    tok_send,
    tok_recv,
    rim_send,
    rim_recv,
    part_send,
    mate_recv,
    part_recv,
    load,
    stat_send,
    stat_recv,
):
    f32, bf16 = jnp.float32, jnp.bfloat16
    me, t = lax.axis_index("sp"), lax.axis_index("tp")
    rows = tok_ref.shape[0]
    seq_len = rows * n
    half_n = n // 2
    column = me % 2
    pos = (me // 2) * (1 - column) + column * (n - 1 - me // 2)

    def at(p):
        p = lax.rem(p + n, n)
        back = p // half_n
        return (1 - back) * (2 * p) + back * (2 * (n - 1 - p) + 1)

    ring = (at(pos + 1), at(pos - 1))
    after, before = lax.rem(me + 1, n), lax.rem(me + n - 1, n)
    mate = t + 1 - 2 * lax.rem(t, 2)
    across = lax.rem(t + 2, tp)
    per = n // tp

    def rdma(src, dst, send, recv, sp, tpi):
        return pltpu.make_async_remote_copy(
            src_ref=src,
            dst_ref=dst,
            send_sem=send,
            recv_sem=recv,
            device_id={"sp": sp, "tp": tpi},
            device_id_type=MESH,
        )

    qc, kc = wq_ref.shape[1], wk_ref.shape[0]
    cc = wc_ref.shape[1]
    depth = wq_ref.shape[0]
    hd = depth // 2
    barrier = pltpu.get_barrier_semaphore()
    peers = [(s, t) for s in ring] + [(s, t) for s in (before, after)]
    peers += [(me, lax.rem(t + i, tp)) for i in range(1, tp)]
    for s, p in peers:
        pl.semaphore_signal(barrier, inc=1, device_id={"sp": s, "tp": p}, device_id_type=MESH)

    loads = []

    def fetch(src, dst):
        copy = pltpu.make_async_copy(src, dst, load.at[len(loads)])
        copy.start()
        loads.append(copy)

    for h in range(2):
        fetch(wq_ref.at[pl.ds(h * hd, hd)], win.at[me, h, :, pl.ds(0, qc)])
        fetch(wc_ref.at[pl.ds(h * hd, hd)], win.at[me, h, :, pl.ds(qc + 2 * kc, cc)])
    for b in range(per):
        fetch(tok_ref.at[:, pl.ds(b * depth, depth)], tok.at[t * per + b])
    fetch(woa_ref, wout.at[me, 0])
    fetch(wop_ref, wout.at[me, 1])
    pair = jnp.transpose(jnp.concatenate([wk_ref[...], wv_ref[...]], axis=0).astype(f32)).astype(bf16)
    for h in range(2):
        win[me, h, :, qc : qc + 2 * kc] = pair[h * hd : (h + 1) * hd]
    for copy in loads:
        copy.wait()
    pl.semaphore_wait(barrier, len(peers))

    def ring_copy(buf, send, recv, way, k, hop):
        sign = -1 if way == 0 else 1
        h = k % 2 if way == 0 else 1 - k % 2
        slot = buf.at[at(pos + sign * (k // 2 + hop)), h]
        return rdma(slot, slot, send.at[way, k], recv.at[way, k], ring[way], t)

    def w_in(way, k, hop):
        return ring_copy(win, win_send, win_recv, way, k, hop)

    def w_out(way, k, hop):
        return ring_copy(wout, wout_send, wout_recv, way, k, hop)

    def tok_copy(owner, b, i, dst):
        slot = tok.at[owner * per + b]
        return rdma(slot, slot, tok_send.at[i], tok_recv.at[i], me, dst)

    for b in range(per):
        tok_copy(t, b, b, across).start()
        for way in range(2):
            if b < 2:
                w_in(way, b, 0).start()
    for b in range(per):
        tok_copy(t, b, per + b, mate).start()

    last = n - 2
    origin = [at(pos)]
    for d in range(1, half_n):
        origin += [at(pos - d), at(pos + d)]
    origin.append(at(pos + half_n))

    def project(i, first=False):
        o = origin[i]
        w = win[o].reshape(depth, qc + 2 * kc + cc)
        term = jnp.dot(tok[o], w, preferred_element_type=f32)
        if first:
            acc[...] = term
        else:
            acc[...] += term

    def relay(copy, k, after_last):
        for way in range(2):
            copy(way, k, 1).wait_recv()
            if k + 2 <= last:
                copy(way, k + 2, 0).start()
            elif after_last is not None:
                after_last(way, k + 1 - last)

    def start_out(way, k):
        w_out(way, k, 0).start()

    ready = 0
    done_blocks = 0
    tok_step = {1: 0, 3: 1}
    tokens_here = False
    for k in range(last + 1):
        relay(w_in, k, start_out)
        if k in tok_step:
            b = tok_step[k]
            tok_copy(across, b, b, across).wait_recv()
            tok_copy(across, b, 2 * per + b, mate).start()
        if k == 3:
            for b in range(per):
                tok_copy(mate, b, per + b, mate).wait_recv()
                tok_copy(lax.rem(mate + 2, tp), b, 2 * per + b, mate).wait_recv()
            tokens_here = True
        ready = 1 + 2 * ((k + 1) // 2) if k < last else n
        if tokens_here:
            while done_blocks < ready and (k == last or done_blocks < 1 + 2 * ((k - 2) // 1)):
                project(done_blocks, done_blocks == 0)
                done_blocks += 1

    query[...] = acc[:, 0:qc].astype(bf16)
    kv[WINDOW : WINDOW + rows, :] = acc[:, qc : qc + 2 * kc].astype(bf16)
    chan[RIM : RIM + rows, :] = acc[:, qc + 2 * kc :].astype(bf16)

    def rim(buf, width, down, i):
        if down:
            return rdma(buf.at[pl.ds(rows, width)], buf.at[pl.ds(0, width)], rim_send.at[i], rim_recv.at[i], after, t)
        return rdma(
            buf.at[pl.ds(width, width)], buf.at[pl.ds(rows + width, width)], rim_send.at[i], rim_recv.at[i], before, t
        )

    rims = [rim(kv, WINDOW, True, 0), rim(kv, WINDOW, False, 1), rim(chan, RIM, True, 2), rim(chan, RIM, False, 3)]
    for c in rims:
        c.start()

    group = qc // kc

    def attend(b):
        band = kv[b * WINDOW : (b + 3) * WINDOW, :]
        q = query[b * WINDOW : (b + 1) * WINDOW, :]
        stacked = jnp.concatenate([q[:, g * HEAD_DIM : (g + 1) * HEAD_DIM] for g in range(group)], axis=0)
        scores = lax.dot_general(
            stacked, band[:, :HEAD_DIM], (((1,), (1,)), ((), ())), preferred_element_type=f32
        ) * HEAD_DIM ** (-0.5)
        scores = scores.reshape(group, WINDOW, 3 * WINDOW)
        r = lax.broadcasted_iota(jnp.int32, (WINDOW, 3 * WINDOW), 0)
        c = lax.broadcasted_iota(jnp.int32, (WINDOW, 3 * WINDOW), 1)
        keep = (c >= r) & (c <= r + 2 * WINDOW)
        key_pos = c + (me * rows + b * WINDOW - WINDOW)
        keep = keep & (key_pos >= 0) & (key_pos < seq_len)
        outs = []
        for g in range(group):
            s = jnp.where(keep, scores[g], masked_score)
            logit = sink_ref[0, g]
            top = jnp.maximum(jnp.max(s, axis=1, keepdims=True), logit)
            raised = jnp.exp(s - top)
            total = jnp.sum(raised, axis=1, keepdims=True) + jnp.exp(logit - top)
            outs.append((raised * (1.0 / total)).astype(bf16))
        got = jnp.dot(jnp.concatenate(outs, axis=0), band, preferred_element_type=f32)
        got = got[:, HEAD_DIM : 2 * HEAD_DIM].astype(bf16)
        hidden[b * WINDOW : (b + 1) * WINDOW, 0:qc] = jnp.concatenate(
            [got[g * WINDOW : (g + 1) * WINDOW] for g in range(group)], axis=1
        )

    def pool():
        length = rows + 2 * RIM
        e = chan[...].astype(f32)
        p = lax.broadcasted_iota(jnp.int32, (length, 1), 0) + (me * rows - RIM)
        e = jnp.where((p >= 0) & (p < seq_len), e, 0.0)
        sums = e + pltpu.roll(e, 1, 0)
        pick = sums
        for level in range(1, POOL_GROUPS):
            step = 2 ** (level - 1)
            sums = pltpu.roll(sums, step, 0) + pltpu.roll(sums, length - step, 0)
            pick = jnp.where(t == level, sums, pick)
        half = 1
        for level in range(1, POOL_GROUPS):
            half = jnp.where(t == level, 2**level, half)
        count = (jnp.clip(p + half, 0, seq_len) - jnp.clip(p - half, 0, seq_len)).astype(f32)
        spread = (pick[RIM : RIM + rows] / count[RIM : RIM + rows] - e[RIM : RIM + rows]).astype(bf16)
        got = jnp.dot(spread, wp_ref[0], preferred_element_type=f32)
        hidden[:, qc:] = (got * ps_ref[...]).astype(bf16)

    def to_mate(o):
        return rdma(part.at[o], mated.at[o], part_send.at[o], mate_recv.at[o], me, mate)

    def to_owner(o):
        s = lax.rem(o, per)
        return rdma(part.at[o], landed.at[s], part_send.at[o], part_recv.at[s], me, across)

    def emit(i):
        o = origin[i]
        got = jnp.dot(hidden[:, 0:qc], wout[o, 0], preferred_element_type=f32)
        got = got + jnp.dot(hidden[:, qc:], wout[o, 1], preferred_element_type=f32)
        part[o] = got.astype(bf16)

        @pl.when(lax.rem(o // per, 2) != lax.rem(t, 2))
        def _():
            to_mate(o).start()

    def combine(i):
        o = origin[i]

        @pl.when(o // per == t)
        def _():
            to_mate(o).wait_recv()
            own[lax.rem(o, per)] = part[o].astype(f32) + mated[o].astype(f32)

        @pl.when(o // per == across)
        def _():
            to_mate(o).wait_recv()
            part[o] = (part[o].astype(f32) + mated[o].astype(f32)).astype(bf16)
            to_owner(o).start()

    blocks = rows // WINDOW
    relay(w_out, 0, None)
    for b in range(1, blocks - 1):
        attend(b)
    relay(w_out, 1, None)
    for c in rims:
        c.wait()
    pool()
    relay(w_out, 2, None)
    attend(0)
    relay(w_out, 3, None)
    attend(blocks - 1)
    for i in range(0, 5):
        emit(i)
    for i in range(0, 5):
        combine(i)
    for k in range(4, last + 1):
        relay(w_out, k, None)
        if k % 2 == 1:
            emit(k)
            emit(k + 1)
            combine(k)
            combine(k + 1)
    emit(n - 1)
    combine(n - 1)

    share = []
    for s in range(per):
        to_owner(t * per + s).wait_recv()
        share.append(own[s] + landed[s].astype(f32))
    mix = jnp.concatenate(share, axis=1)
    acc[:, 0 : mix.shape[1]] = mix
    one = jnp.sum(mix, axis=1, keepdims=True)
    two = jnp.sum(mix * mix, axis=1, keepdims=True)
    lane = lax.broadcasted_iota(jnp.int32, (rows, 128), 1)
    both = jnp.where(lane == 0, one, jnp.where(lane == 1, two, 0.0))
    stats[t] = jnp.transpose(both)[0:8]

    def stat_copy(j):
        return rdma(stats.at[t], stats.at[t], stat_send.at[j], stat_recv.at[t], me, lax.rem(t + j, tp))

    for j in range(1, tp):
        stat_copy(j).start()
    for o in range(n):

        @pl.when(o // per != t)
        def _():
            to_mate(o).wait_send()

    for k in range(last + 1):
        for way in range(2):
            w_in(way, k, 0).wait_send()
            w_out(way, k, 0).wait_send()
    for b in range(per):
        tok_copy(t, b, b, across).wait_send()
        tok_copy(t, b, per + b, mate).wait_send()
        tok_copy(across, b, 2 * per + b, mate).wait_send()
    for j in range(1, tp):
        src = lax.rem(t + j, tp)
        rdma(stats.at[src], stats.at[src], stat_send.at[j], stat_recv.at[src], me, src).wait_recv()
    totals = stats[0]
    for i in range(1, tp):
        totals = totals + stats[i]
    wide = jnp.concatenate([totals, jnp.zeros((120, rows), f32)], axis=0)
    back = jnp.transpose(wide)
    width = gain_ref.shape[1] * tp
    row_mean = back[:, 0:1] / width
    variance = back[:, 1:2] / width - row_mean * row_mean
    scale = lax.rsqrt(variance + epsilon)
    out_ref[...] = ((acc[:, 0 : gain_ref.shape[1]] - row_mean) * scale * gain_ref[...]).astype(bf16)
    for j in range(1, tp):
        stat_copy(j).wait_send()


def fused(n, tp, tokens, w_query, w_key, w_value, w_pool_in, sink, w_pool, pool_scale, w_out_attn, w_out_pool, out_gain):
    rows, share = tokens.shape
    depth, qc = w_query.shape
    kc, cc = w_key.shape[1], w_pool_in.shape[1]
    wide = w_out_attn.shape[1]
    per = n // tp
    bf16, f32 = jnp.bfloat16, jnp.float32
    dma = pltpu.SemaphoreType.DMA
    vmem = pl.BlockSpec(memory_space=pltpu.VMEM)
    specs = [vmem] * 11
    specs[5] = pl.BlockSpec(memory_space=pltpu.SMEM)
    for i in (0, 1, 4, 8, 9):
        specs[i] = pl.BlockSpec(memory_space=pl.ANY)
    return pl.pallas_call(
        functools.partial(mixer_kernel, n, tp),
        out_shape=jax.ShapeDtypeStruct((rows, share), bf16),
        in_specs=specs,
        out_specs=vmem,
        scratch_shapes=[
            pltpu.VMEM((n, 2, depth // 2, qc + 2 * kc + cc), bf16),
            pltpu.VMEM((n, 2, qc, wide), bf16),
            pltpu.VMEM((n, rows, depth), bf16),
            pltpu.VMEM((rows, qc + 2 * kc + cc), f32),
            pltpu.VMEM((rows, qc), bf16),
            pltpu.VMEM((rows + 2 * WINDOW, 2 * kc), bf16),
            pltpu.VMEM((rows + 2 * RIM, cc), bf16),
            pltpu.VMEM((rows, qc + cc), bf16),
            pltpu.VMEM((n, rows, wide), bf16),
            pltpu.VMEM((n, rows, wide), bf16),
            pltpu.VMEM((per, rows, wide), bf16),
            pltpu.VMEM((per, rows, wide), f32),
            pltpu.VMEM((tp, 8, rows), f32),
            dma((2, n - 1)),
            dma((2, n - 1)),
            dma((2, n - 1)),
            dma((2, n - 1)),
            dma((3 * per,)),
            dma((3 * per,)),
            dma((4,)),
            dma((4,)),
            dma((n,)),
            dma((n,)),
            dma((per,)),
            dma((6 + per,)),
            dma((tp,)),
            dma((tp,)),
        ],
        compiler_params=pltpu.CompilerParams(
            collective_id=0, has_side_effects=True, vmem_limit_bytes=60 * 1024 * 1024
        ),
        name="mixer",
    )(
        tokens,
        w_query,
        w_key.T,
        w_value.T,
        w_pool_in,
        sink.reshape(1, -1),
        w_pool,
        pool_scale.reshape(1, -1),
        w_out_attn,
        w_out_pool,
        out_gain.reshape(1, -1),
    )


def fits(n, tp, tokens, w_query, w_key, w_pool, w_out_attn):
    return (
        tp == 4
        and n == 2 * tp
        and w_query.shape[0] % 32 == 0
        and w_query.shape[1] % 128 == 0
        and w_key.shape[1] == HEAD_DIM
        and w_pool.shape[0] == 1
        and w_out_attn.shape[1] % 128 == 0
        and tokens.shape[0] >= 2 * WINDOW
    )


def mixed_rows(*args):
    n, tp = lax.axis_size("sp"), lax.axis_size("tp")
    if fits(n, tp, args[0], args[1], args[2], args[6], args[8]):
        return fused(n, tp, *args)
    return local(*args)


def solution(mesh):
    return jax.shard_map(
        mixed_rows,
        mesh=mesh,
        in_specs=(
            P("sp", "tp"),
            P("sp", "tp"),
            P("sp", "tp"),
            P("sp", "tp"),
            P("sp", "tp"),
            P("tp"),
            P("tp", None, None),
            P("tp"),
            P("tp", "sp"),
            P("tp", "sp"),
            P("tp"),
        ),
        out_specs=P("sp", "tp"),
        check_vma=False,
    )
```
